256 devices in a mesh: rep: 2 (over z_hi), fs: 16 (over z_lo, x), tp: 8 (over y, core).
Axes of the slice: x: 4, y: 4, z: 8 (z_hi: 2, z_lo: 4; z = z_hi * 4 + z_lo), core: 2. Of those that a mesh axis runs over, the one named last changes fastest.
Arguments:
- tokens: bfloat16 [32768, 2048], P(('rep', 'fs', 'tp')), may hold values from -6 to 6
- cotangent: bfloat16 [32768, 2048], P(('rep', 'fs', 'tp')), may hold values from -24 to 24
- gate_weight: bfloat16 [2048, 3072], P('fs', 'tp'), may hold values from -0.125 to 0.125
- up_weight: bfloat16 [2048, 3072], P('fs', 'tp'), may hold values from -0.125 to 0.125
- down_weight: bfloat16 [3072, 2048], P('tp', 'fs'), may hold values from -0.109375 to 0.109375
Outputs:
- grad_tokens: bfloat16 [32768, 2048], P(('rep', 'fs', 'tp'))
- grad_gate: float32 [2048, 3072], P('fs', 'tp')
- grad_up: float32 [2048, 3072], P('fs', 'tp')
- grad_down: float32 [3072, 2048], P('tp', 'fs')
- gate_row_norms: float32 [2048], P('fs')
- up_row_norms: float32 [2048], P('fs')
- down_row_norms: float32 [3072], P('tp')
The draws below stay inside these ranges and needn't reach their ends.
All inputs are finite; a program needn't handle non-finite values.
Results may differ from the reference program's by a relative error of at most 0.014.
Values may be sent and summed in bfloat16 or wider, within the bound.
No kernel may reach another device: no remote copies, remote signals or barrier semaphores. Data moves between devices by JAX's collectives and lax.ppermute only.
A program may use at most 128 MiB of HBM per device.

```python
import jax
import jax.numpy as jnp
from jax import lax

D = 2048
FF = 3072
TOKENS = 32768
N_TP = 8


def strengthened(entries, stream_key, source, target, blocks, factor):
    owner, partner = [(jnp.arange(entries.shape[dim]) // (entries.shape[dim] // blocks)).reshape([-1 if axis == dim else 1 for axis in range(entries.ndim)]) for dim in (source, target)]
    chosen = jax.random.permutation(stream_key, blocks)[partner]
    strong = (owner == chosen) | (owner == (partner + blocks // 2) % blocks)
    return jnp.where(strong, factor * entries, entries)


def shard_levels(rng, dims, pieces, low, largest):
    factor_of, own = 1.0, jax.random.fold_in(rng, 6)
    for dim, parts in pieces:
        draws = jnp.exp(jax.random.uniform(jax.random.fold_in(own, dim), (parts,), jnp.float32, low / len(pieces), largest / len(pieces)))
        factor_of = factor_of * jnp.repeat(draws, dims[dim] // parts).reshape([-1 if axis == dim else 1 for axis in range(len(dims))])
    return factor_of


def centred(stream_key, dims, scale, reach, cuts=(), held_as=jnp.bfloat16):
    loudness = shard_levels(stream_key, dims, cuts, -0.22, 0.18) if cuts else 1.0
    drawn = jax.random.normal(stream_key, dims, jnp.float32) * scale * loudness
    return jnp.minimum(jnp.maximum(drawn, -reach), reach).astype(held_as)


def gaussian_with(key, extent, spread, most, pieces, heavy, dtype=jnp.bfloat16):
    drawn = spread * jax.random.normal(key, extent, jnp.float32)
    if pieces:
        drawn = drawn * shard_levels(key, extent, pieces, -0.22, 0.18)
    return jnp.clip(strengthened(drawn, jax.random.fold_in(key, 3), *heavy), -most, most).astype(dtype)


def setup_inputs(seed: int = 0) -> dict:
    arg_keys = jax.random.split(jax.random.key(seed), 6)
    return {
        "tokens": centred(arg_keys[0], (TOKENS, D), 1.0, 6.0, ((0, 256),)),
        "cotangent": gaussian_with(arg_keys[1], (TOKENS, D), 1.0, 24.0, ((0, 256),), (0, 1, 256, 6.0)),
        "gate_weight": centred(arg_keys[2], (D, FF), D ** -0.5, 0.125, ((0, 16), (1, 8))),
        "up_weight": centred(arg_keys[3], (D, FF), D ** -0.5, 0.125, ((0, 16), (1, 8))),
        "down_weight": centred(arg_keys[4], (FF, D), FF ** -0.5, 0.109375, ((0, 8), (1, 16))),
    }


def reference(tokens, cotangent, gate_weight, up_weight, down_weight):
    gate = jnp.dot(tokens, gate_weight, preferred_element_type=jnp.float32)
    up = jnp.dot(tokens, up_weight, preferred_element_type=jnp.float32)
    sig = jax.nn.sigmoid(gate)
    act = gate * sig
    hidden = (act * up).astype(jnp.bfloat16)
    dhid = jnp.dot(cotangent, down_weight.T, preferred_element_type=jnp.float32)
    dgate = (dhid * up * sig * (1.0 + gate * (1.0 - sig))).astype(jnp.bfloat16)
    dup = (dhid * act).astype(jnp.bfloat16)
    grad_down = jnp.dot(hidden.T, cotangent, preferred_element_type=jnp.float32)
    grad_gate = jnp.dot(tokens.T, dgate, preferred_element_type=jnp.float32)
    grad_up = jnp.dot(tokens.T, dup, preferred_element_type=jnp.float32)
    block_width = FF // N_TP
    total = jnp.zeros(tokens.shape, jnp.float32)
    for block in range(N_TP):
        lower = block * block_width
        upper = lower + block_width
        partial_term = jnp.dot(dgate[:, lower:upper], gate_weight[:, lower:upper].T, preferred_element_type=jnp.float32)
        partial_term = partial_term + jnp.dot(dup[:, lower:upper], up_weight[:, lower:upper].T, preferred_element_type=jnp.float32)
        rounded = lax.optimization_barrier(partial_term.astype(jnp.bfloat16))
        total = total + rounded.astype(jnp.float32)
    grad_tokens = total.astype(jnp.bfloat16)
    gate_row_norms = jnp.sum(grad_gate * grad_gate, axis=1)
    up_row_norms = jnp.sum(grad_up * grad_up, axis=1)
    down_row_norms = jnp.sum(grad_down * grad_down, axis=1)
    return (grad_tokens, grad_gate, grad_up, grad_down, gate_row_norms, up_row_norms, down_row_norms)
```

```python
import functools

import jax
import jax.numpy as jnp
from jax import lax
from jax.experimental import pallas as pl
from jax.experimental.pallas import tpu as pltpu
from jax.sharding import PartitionSpec as P


ALL = ("rep", "fs", "tp")
BF16 = jnp.bfloat16
F32 = jnp.float32


def place(z, x, y, c):
    return (z // 4) * 128 + (z % 4) * 32 + x * 8 + y * 2 + c


def shift(array, dz=0, dx=0, dy=0, dc=0):
    pairs = [
        (place(z, x, y, c), place((z + dz) % 8, (x + dx) % 4, (y + dy) % 4, (c + dc) % 2))
        for z in range(8)
        for x in range(4)
        for y in range(4)
        for c in range(2)
    ]
    return lax.ppermute(array, ALL, pairs)


VMEM = pl.BlockSpec(memory_space=pltpu.VMEM)
SMEM = pl.BlockSpec(memory_space=pltpu.SMEM)
PARAMS = pltpu.CompilerParams(vmem_limit_bytes=56 * 1024 * 1024)


def shape(dims, dtype=BF16):
    return jax.ShapeDtypeStruct(dims, dtype)


def dot(left, right, dims=(1, 0)):
    return lax.dot_general(
        left, right, (((dims[0],), (dims[1],)), ((), ())), preferred_element_type=F32
    )


def front(where, *refs):
    a, refs = refs[:4], refs[4:]
    b, refs = refs[:5], refs[5:]
    tok, cot, refs = refs[:8], refs[8:16], refs[16:]
    toks, cots, wg, wu, hidden, dgate, dup, wd = refs
    x, z = where[0], where[1]
    for xd in range(4):
        for zd in range(4):
            at = ((z + zd) % 4) * 4 + (x + xd) % 4
            for k, w in enumerate((wg, wu, wd)):
                w[at, 0:64, :] = a[xd][zd, k]
                if zd == 2:
                    w[at, 64:128, :] = b[2 + xd // 2][xd % 2, k]
                else:
                    w[at, 64:128, :] = b[(0, 1, 0, 4)[zd]][xd, k]
    for i in range(8):
        toks[i * 128 : (i + 1) * 128, :] = tok[i][...]
        cots[i * 128 : (i + 1) * 128, :] = cot[i][...]
    g_w, u_w, d_w = (w[...].reshape(2048, 384) for w in (wg, wu, wd))
    for i in range(4):
        rows = slice(i * 256, (i + 1) * 256)
        t = toks[rows, :]
        gate = dot(t, g_w)
        up = dot(t, u_w)
        dhid = dot(cots[rows, :], d_w)
        sig = 1.0 / (1.0 + jnp.exp(-gate))
        act = gate * sig
        hidden[rows, :] = (act * up).astype(BF16)
        dgate[rows, :] = (dhid * up * sig * (1.0 + gate * (1.0 - sig))).astype(BF16)
        dup[rows, :] = (dhid * act).astype(BF16)


def weight_grad(z_first, where, left, right, *refs):
    outs, acc = refs[:-1], refs[-1]
    x, z = where[0], where[1]
    lt = left[...].T
    for j in range(8):
        part = dot(lt, right[:, j * 256 : (j + 1) * 256]).astype(BF16)
        for h in range(2):
            s = 2 * j + h
            zd, xd = (s // 4 - z) % 4, (s % 4 - x) % 4
            at = zd * 4 + xd if z_first else xd * 4 + zd
            acc[at] = part[:, h * 128 : (h + 1) * 128]
    at = 0
    for o in outs:
        o[...] = acc[at : at + o.shape[0]]
        at += o.shape[0]


def rows_grad(dgate, dup, wg, wu, mine, other):
    g_w, u_w = (w[...].reshape(2048, 384) for w in (wg, wu))
    for i in range(8):
        rows = slice(i * 128, (i + 1) * 128)
        part = dot(dgate[rows, :], g_w, (1, 1)) + dot(dup[rows, :], u_w, (1, 1))
        (mine, other)[i // 4][i % 4] = part.astype(BF16)


def call(kernel, n_in, outs, scratch=(), where=True):
    return pl.pallas_call(
        kernel,
        out_shape=outs,
        in_specs=([SMEM] if where else []) + [VMEM] * n_in,
        out_specs=[VMEM] * len(outs),
        scratch_shapes=scratch,
        compiler_params=PARAMS,
    )


def total(parts):
    out = parts[0].astype(F32)
    for p in parts[1:]:
        out = out + p.astype(F32)
    return out


def gathered_rows(own):
    below, above = shift(own, dy=1), shift(own, dy=-1)
    return below, above


def sum_over(array, axis):
    count = lax.axis_size(axis)
    got = lax.all_to_all(
        jnp.broadcast_to(array[None], (count, *array.shape)), axis, 0, 0, tiled=True
    )
    return jnp.sum(got, axis=0)


def local(tokens, cotangent, gate_weight, up_weight, down_weight):
    fs = lax.axis_index("fs")
    where = jnp.stack([fs % 4, fs // 4]).astype(jnp.int32)

    tok_b, tok_a = shift(tokens, dy=1), shift(tokens, dy=-1)
    cot_b, cot_a = shift(cotangent, dy=1), shift(cotangent, dy=-1)
    weights = jnp.stack([gate_weight, up_weight, down_weight.T])
    first, second = weights[:, :64], weights[:, 64:]
    a_far = jnp.concatenate([shift(first[:, :32], dz=2), shift(first[:, 32:], dz=-2)], axis=1)
    a_up, a_dn = shift(first, dz=-1), shift(first, dz=1)
    b_far, b_up, b_dn = shift(second, dx=2), shift(second, dx=-1), shift(second, dx=1)
    a4 = jnp.stack([first, a_up, a_far, a_dn])
    b4 = jnp.stack([second, b_up, b_far, b_dn])
    tok_f, cot_f = shift(tok_b, dy=1), shift(cot_a, dy=-1)
    a = (a4, shift(a4, dx=-1), shift(a4, dx=2), shift(a4, dx=1))
    b = (
        b4,
        shift(b4, dz=-1),
        shift(b4[:2], dz=2),
        shift(b4[2:], dz=-2),
        shift(b4, dz=1),
    )
    tok = [tokens, tok_b, tok_a, tok_f]
    cot = [cotangent, cot_b, cot_a, cot_f]
    tok += [shift(t, dc=1) for t in tok]
    cot += [shift(t, dc=1) for t in cot]

    toks, cots, wg, wu, hidden, dgate, dup = call(
        front,
        25,
        [shape((1024, 2048))] * 2 + [shape((16, 128, 384))] * 2 + [shape((1024, 384))] * 3,
        [pltpu.VMEM((16, 128, 384), BF16)],
    )(where, *a, *b, *tok, *cot)

    block = lambda n: shape((n, 384, 128))
    acc = [pltpu.VMEM((16, 384, 128), BF16)]
    z_pieces = [block(4), block(4), block(2), block(2), block(4)]
    x_pieces = [block(4)] * 4
    gate_p = call(functools.partial(weight_grad, False), 2, x_pieces, acc)(where, dgate, toks)
    up_p = call(functools.partial(weight_grad, False), 2, x_pieces, acc)(where, dup, toks)
    down_p = call(functools.partial(weight_grad, True), 2, z_pieces, acc)(where, hidden, cots)

    def over_x(p):
        return total([p[0], shift(p[1], dx=1), shift(p[2], dx=2), shift(p[3], dx=-1)])

    def over_z(p):
        far = jnp.concatenate([shift(p[2], dz=2), shift(p[3], dz=-2)])
        return total([p[0], shift(p[1], dz=1), far, shift(p[4], dz=-1)])

    def over_rep(p):
        p = p.astype(BF16)
        return total([p, shift(p, dz=4)])

    def x_then_z(p):
        s = over_x(p).astype(BF16)
        return over_rep(over_z((s[0], s[1], s[2, :192], s[2, 192:], s[3])))

    def z_then_x(p):
        s = over_z(p).astype(BF16)
        return over_rep(over_x(s))

    down_t = z_then_x(down_p)
    gate_t = x_then_z(gate_p)
    up_t = x_then_z(up_p)

    mine, other = call(rows_grad, 4, [shape((4, 128, 2048))] * 2, where=False)(dgate, dup, wg, wu)
    both = total([mine, shift(other, dc=1)]).astype(BF16)
    grad_tokens = total(
        [both[0], shift(both[1], dy=-1), shift(both[2], dy=1), shift(both[3], dy=2)]
    ).astype(BF16)

    norms = sum_over(
        jnp.concatenate([jnp.sum(gate_t * gate_t, axis=0), jnp.sum(up_t * up_t, axis=0)]), "tp"
    )
    down_norms = sum_over(jnp.sum(down_t * down_t, axis=1), "fs")
    return grad_tokens, gate_t.T, up_t.T, down_t, norms[:128], norms[128:], down_norms


def solution(mesh):
    return jax.shard_map(
        local,
        mesh=mesh,
        in_specs=(P(ALL, None), P(ALL, None), P("fs", "tp"), P("fs", "tp"), P("tp", "fs")),
        out_specs=(
            P(ALL, None),
            P("fs", "tp"),
            P("fs", "tp"),
            P("tp", "fs"),
            P("fs"),
            P("fs"),
            P("tp"),
        ),
        check_vma=False,
    )
```
